32 devices in a mesh: fs: 8 (over z, y), tp: 4 (over x, core).
Axes of the slice: x: 2, y: 2, z: 4, core: 2. Of those that a mesh axis runs over, the one named last changes fastest.
Arguments:
- normed_input: bfloat16 [8192, 4096], P('fs'), may hold values from -6 to 6
- query_cotangent: bfloat16 [8192, 2048], P('fs', 'tp'), may hold values from -40 to 40
- key_cotangent: bfloat16 [8192, 2048], P('fs', 'tp'), may hold values from -40 to 40
- head_outputs: bfloat16 [8192, 2048], P('fs', 'tp'), may hold values from -40 to 40
- output_cotangent: bfloat16 [8192, 4096], P('fs'), may hold values from -6 to 6
- query_basis: bfloat16 [4096, 256], P('fs'), may hold values from -2.5 to 2.5
- key_basis: bfloat16 [4096, 256], P('fs'), may hold values from -2.5 to 2.5
- output_basis: bfloat16 [4096, 256], P('fs'), may hold values from -2.5 to 2.5
- query_master: float32 [4096, 2048], P('fs', 'tp'), may hold values from -6 to 6
- key_master: float32 [4096, 2048], P('fs', 'tp'), may hold values from -6 to 6
- output_master: float32 [2048, 4096], P('tp', 'fs'), may hold values from -6 to 6
- query_first: float32 [256, 2048], P('fs', 'tp'), may hold values from -6 to 6
- query_second: float32 [256, 2048], P('fs', 'tp'), may hold values from 0.05 to 0.5
- key_first: float32 [256, 2048], P('fs', 'tp'), may hold values from -6 to 6
- key_second: float32 [256, 2048], P('fs', 'tp'), may hold values from 0.05 to 0.5
- output_first: float32 [256, 2048], P('fs', 'tp'), may hold values from -6 to 6
- output_second: float32 [256, 2048], P('fs', 'tp'), may hold values from 0.05 to 0.5
Outputs:
- query_master_new: float32 [4096, 2048], P('fs', 'tp')
- key_master_new: float32 [4096, 2048], P('fs', 'tp')
- output_master_new: float32 [2048, 4096], P('tp', 'fs')
- query_copy: bfloat16 [4096, 2048], P(None, 'tp')
- key_copy: bfloat16 [4096, 2048], P(None, 'tp')
- output_copy: bfloat16 [2048, 4096], P('tp')
- query_step: bfloat16 [4096, 2048], P('fs', 'tp')
- key_step: bfloat16 [4096, 2048], P('fs', 'tp')
- output_step: bfloat16 [2048, 4096], P('tp', 'fs')
- query_first_new: float32 [256, 2048], P('fs', 'tp')
- query_second_new: float32 [256, 2048], P('fs', 'tp')
- key_first_new: float32 [256, 2048], P('fs', 'tp')
- key_second_new: float32 [256, 2048], P('fs', 'tp')
- output_first_new: float32 [256, 2048], P('fs', 'tp')
- output_second_new: float32 [256, 2048], P('fs', 'tp')
The draws below stay inside these ranges and needn't reach their ends.
All inputs are finite; a program needn't handle non-finite values.
Results may differ from the reference program's by a relative error of at most 0.007.
Values may be sent and summed in bfloat16 or wider, within the bound.
A program may use at most 128 MiB of HBM per device.

```python
import math
import jax
import jax.numpy as jnp
from jax import lax

D = 4096
RANK = 256
C_W = 2048
TOKENS = 8192


def column_scaled(key, rows, cols):
    noise_key, scale_key = jax.random.split(key)
    values = jnp.clip(jax.random.normal(noise_key, (rows, cols), jnp.float32), -4.0, 4.0)
    ramp = jnp.arange(cols, dtype=jnp.float32) / max(cols - 1, 1)
    jitter = jax.random.uniform(scale_key, (cols,), jnp.float32, -0.35, 0.35)
    scales = jnp.exp(math.log(4.0) * ramp + jitter)
    return values * scales[None, :]


def draw_query_cotangent(key, part):
    return column_scaled(jax.random.fold_in(key, 11), TOKENS, C_W).astype(jnp.bfloat16)


def draw_key_cotangent(key, part):
    return column_scaled(jax.random.fold_in(key, 12), TOKENS, C_W).astype(jnp.bfloat16)


def draw_head_outputs(key, part):
    return column_scaled(jax.random.fold_in(key, 13), TOKENS, C_W).astype(jnp.bfloat16)


def draw_query_basis(key, part):
    return (column_scaled(jax.random.fold_in(key, 21), D, RANK) * RANK ** (-0.5)).astype(jnp.bfloat16)


def draw_key_basis(key, part):
    return (column_scaled(jax.random.fold_in(key, 22), D, RANK) * RANK ** (-0.5)).astype(jnp.bfloat16)


def draw_output_basis(key, part):
    return (column_scaled(jax.random.fold_in(key, 23), D, RANK) * RANK ** (-0.5)).astype(jnp.bfloat16)


def shard_levels(rng, extent, shards, smallest, top_value):
    level, own = 1.0, jax.random.fold_in(rng, 6)
    for position, parts in shards:
        steps = jnp.exp(jax.random.uniform(jax.random.fold_in(own, position), (parts,), jnp.float32, smallest / len(shards), top_value / len(shards)))
        level = level * jnp.repeat(steps, extent[position] // parts).reshape([-1 if axis == position else 1 for axis in range(len(extent))])
    return level


def noise(stream_key, extent, scale, most, cuts=(), kind=jnp.bfloat16):
    values = jax.random.normal(stream_key, extent, jnp.float32) * scale
    if len(cuts) > 0:
        values = shard_levels(stream_key, extent, cuts, -0.22, 0.18) * values
    return jnp.clip(values, min=-most, max=most).astype(kind)


def setup_inputs(seed: int = 0) -> dict:
    splits = jax.random.split(jax.random.key(seed), 18)
    return {
        "normed_input": noise(splits[0], (TOKENS, D), 1.0, 6.0, ((0, 8),)),
        "query_cotangent": draw_query_cotangent(jax.random.fold_in(splits[17], 71), 0),
        "key_cotangent": draw_key_cotangent(jax.random.fold_in(splits[17], 71), 0),
        "head_outputs": draw_head_outputs(jax.random.fold_in(splits[17], 71), 0),
        "output_cotangent": noise(splits[4], (TOKENS, D), 1.0, 6.0, ((0, 8),)),
        "query_basis": draw_query_basis(jax.random.fold_in(splits[17], 71), 0),
        "key_basis": draw_key_basis(jax.random.fold_in(splits[17], 71), 0),
        "output_basis": draw_output_basis(jax.random.fold_in(splits[17], 71), 0),
        "query_master": noise(splits[8], (D, C_W), 1.0, 6.0, ((0, 8), (1, 4)), jnp.float32),
        "key_master": noise(splits[9], (D, C_W), 1.0, 6.0, ((0, 8), (1, 4)), jnp.float32),
        "output_master": noise(splits[10], (C_W, D), 1.0, 6.0, ((0, 4), (1, 8)), jnp.float32),
        "query_first": noise(splits[11], (RANK, C_W), 1.0, 6.0, ((0, 8), (1, 4)), jnp.float32),
        "query_second": jnp.clip(jnp.exp(math.log(0.5) - 2.3025851 * jax.random.uniform(splits[12], (RANK, C_W), jnp.float32) ** shard_levels(splits[12], (RANK, C_W), ((0, 8), (1, 4)), -0.2, 0.2)), 0.05, 0.5),
        "key_first": noise(splits[13], (RANK, C_W), 1.0, 6.0, ((0, 8), (1, 4)), jnp.float32),
        "key_second": jnp.clip(jnp.exp(math.log(0.5) - 2.3025851 * jax.random.uniform(splits[14], (RANK, C_W), jnp.float32) ** shard_levels(splits[14], (RANK, C_W), ((0, 8), (1, 4)), -0.2, 0.2)), 0.05, 0.5),
        "output_first": noise(splits[15], (RANK, C_W), 1.0, 6.0, ((0, 8), (1, 4)), jnp.float32),
        "output_second": jnp.clip(jnp.exp(math.log(0.5) - 2.3025851 * jax.random.uniform(splits[16], (RANK, C_W), jnp.float32) ** shard_levels(splits[16], (RANK, C_W), ((0, 8), (1, 4)), -0.2, 0.2)), 0.05, 0.5),
    }


bias_first = 1.0 / (1.0 - 0.8 ** 10)
bias_second = 1.0 / (1.0 - 0.95 ** 10)
learn_rate = 0.05
decay_rate = 0.1

def product(left, right):
    return jnp.dot(left.astype(jnp.float32), right.astype(jnp.float32), precision=lax.Precision.HIGHEST)

def moment_update(first_moment, second_moment, clipped):
    first_new = 0.8 * first_moment + 0.2 * clipped
    second_new = 0.95 * second_moment + 0.05 * clipped * clipped
    direction = first_new * bias_first / (jnp.sqrt(second_new * bias_second) + 1e-08)
    return (first_new, second_new, direction.astype(jnp.bfloat16))

def reference(normed_input, query_cotangent, key_cotangent, head_outputs, output_cotangent, query_basis, key_basis, output_basis, query_master, key_master, output_master, query_first, query_second, key_first, key_second, output_first, output_second):
    query_grad = product(normed_input.T, query_cotangent)
    key_grad = product(normed_input.T, key_cotangent)
    output_grad = product(output_cotangent.T, head_outputs)
    query_low = product(query_basis.T, query_grad)
    key_low = product(key_basis.T, key_grad)
    output_low = product(output_basis.T, output_grad)
    sum_squares = jnp.sum(query_low * query_low) + jnp.sum(key_low * key_low) + jnp.sum(output_low * output_low)
    clip_factor = jnp.minimum(1.0, jnp.sqrt(3.0 * RANK * C_W / sum_squares))
    query_first_new, query_second_new, query_dir = moment_update(query_first, query_second, clip_factor * query_low)
    key_first_new, key_second_new, key_dir = moment_update(key_first, key_second, clip_factor * key_low)
    output_first_new, output_second_new, output_dir = moment_update(output_first, output_second, clip_factor * output_low)
    query_update = 0.25 * product(query_basis, query_dir)
    key_update = 0.25 * product(key_basis, key_dir)
    output_update = 0.25 * product(output_basis, output_dir).T
    query_master_new = query_master - learn_rate * (query_update + decay_rate * query_master)
    key_master_new = key_master - learn_rate * (key_update + decay_rate * key_master)
    output_master_new = output_master - learn_rate * (output_update + decay_rate * output_master)
    return (query_master_new, key_master_new, output_master_new, query_master_new.astype(jnp.bfloat16), key_master_new.astype(jnp.bfloat16), output_master_new.astype(jnp.bfloat16), query_update.astype(jnp.bfloat16), key_update.astype(jnp.bfloat16), output_update.astype(jnp.bfloat16), query_first_new, query_second_new, key_first_new, key_second_new, output_first_new, output_second_new)
```

```python
import functools
import jax
import jax.numpy as jnp
from jax import lax
from jax.experimental import pallas as pl
from jax.experimental.pallas import tpu as pltpu
from jax.sharding import PartitionSpec as P

RANK = 256
C_W = 2048
MESH = pl.DeviceIdType.MESH

bias_first = 1.0 / (1.0 - 0.8**10)
bias_second = 1.0 / (1.0 - 0.95**10)
learn_rate = 0.05
decay_rate = 0.1


def slot(ref, dim, owner, size, part, rows):
    if ref.ndim == 3:
        return ref.at[owner, pl.ds(part * rows, rows), :]
    if dim == 0:
        return ref.at[pl.ds(pl.multiple_of(owner * size + part * rows, 8), rows), :]
    return ref.at[pl.ds(part * rows, rows), pl.ds(pl.multiple_of(owner * size, 128), size)]


def gather_kernel(axis, major, minor, cut, dims, sizes, *refs):
    arrays = len(dims)
    count = arrays * cut
    whole_ins, outs = refs[:arrays], refs[arrays : 2 * arrays]
    (local, up_send, up_recv, down_send, down_recv, side_send, side_recv, pair_send, pair_recv) = refs[
        2 * arrays :
    ]
    heights = [ref.shape[0] // cut for ref in whole_ins]
    ins = [whole_ins[c // cut].at[pl.ds(c % cut * heights[c // cut], heights[c // cut]), :] for c in range(count)]
    ends = {c for c in range(count) if c % 2 and major >= 4 and major % 2 == 0}
    me = lax.axis_index(axis)
    z, y = me // minor, me % minor

    def side_peer(o):
        return z * minor + (y + o) % minor

    barrier = pltpu.get_barrier_semaphore()

    @pl.when(z < major - 1)
    def _():
        pl.semaphore_signal(barrier, inc=1, device_id={axis: me + minor}, device_id_type=MESH)

    @pl.when(z > 0)
    def _():
        pl.semaphore_signal(barrier, inc=1, device_id={axis: me - minor}, device_id_type=MESH)

    for o in range(1, minor):
        pl.semaphore_signal(barrier, inc=1, device_id={axis: side_peer(o)}, device_id_type=MESH)

    later, earlier = (2 * major - 2 - z) // major, (z + major - 1) // major
    pl.semaphore_wait(barrier, later + earlier + minor - 1)

    def at(c, owner):
        a = c // cut
        return slot(outs[a], dims[a], owner, sizes[a], c % cut, heights[a])

    def line(sign, d, c):
        owner = me - sign * d * minor
        send, recv = (up_send, up_recv) if sign > 0 else (down_send, down_recv)
        return pltpu.make_async_remote_copy(
            src_ref=ins[c] if d == 0 else at(c, owner),
            dst_ref=at(c, owner),
            send_sem=send.at[d, c],
            recv_sem=recv.at[d, c],
            device_id={axis: me + sign * minor},
            device_id_type=MESH,
        )

    def line_arrival(sign, d, c):
        owner = me - sign * d * minor
        send, recv = (up_send, up_recv) if sign > 0 else (down_send, down_recv)
        return pltpu.make_async_remote_copy(
            src_ref=at(c, owner),
            dst_ref=at(c, owner),
            send_sem=send.at[d - 1, c],
            recv_sem=recv.at[d - 1, c],
            device_id={axis: me - sign * minor},
            device_id_type=MESH,
        )

    def side(sign, d, o, c):
        owner = me - sign * d * minor
        index = d if sign > 0 else major + d
        return pltpu.make_async_remote_copy(
            src_ref=ins[c] if d == 0 else at(c, owner),
            dst_ref=at(c, owner),
            send_sem=side_send.at[index, o, c],
            recv_sem=side_recv.at[index, o, c],
            device_id={axis: side_peer(o)},
            device_id_type=MESH,
        )

    def side_arrival(sign, d, o, c):
        source = (y + minor - o) % minor
        owner = (z - sign * d) * minor + source
        index = d if sign > 0 else major + d
        return pltpu.make_async_remote_copy(
            src_ref=at(c, owner),
            dst_ref=at(c, owner),
            send_sem=side_send.at[index, o, c],
            recv_sem=side_recv.at[index, o, c],
            device_id={axis: side_peer(o)},
            device_id_type=MESH,
        )

    def takes(sign):
        return z % 2 == (1 if sign > 0 else 0)

    def gives(sign):
        return z % 2 == (0 if sign > 0 else 1)

    def to_pair(sign, o, c):
        owner = z * minor + (y + minor - o) % minor
        return pltpu.make_async_remote_copy(
            src_ref=at(c, owner),
            dst_ref=at(c, owner),
            send_sem=pair_send.at[o, c],
            recv_sem=pair_recv.at[o, c],
            device_id={axis: me + sign * minor},
            device_id_type=MESH,
        )

    def pair_arrival(sign, o, c):
        owner = (z - sign) * minor + (y + minor - o) % minor
        return pltpu.make_async_remote_copy(
            src_ref=at(c, owner),
            dst_ref=at(c, owner),
            send_sem=pair_send.at[o, c],
            recv_sem=pair_recv.at[o, c],
            device_id={axis: me - sign * minor},
            device_id_type=MESH,
        )

    def held(sign, d):
        return z >= d if sign > 0 else z + d < major

    def onward(sign):
        return z < major - 1 if sign > 0 else z > 0

    for c in range(count):
        for sign in (1, -1):
            pl.when(onward(sign))(line(sign, 0, c).start)
        for o in range(1, minor):
            side(1, 0, o, c).start()
    for c in range(count):
        pltpu.make_async_copy(ins[c], at(c, me), local.at[c]).start()
    for d in range(1, major):
        for c in range(count):
            for sign in (1, -1):

                @pl.when(held(sign, d))
                def _(sign=sign, d=d, c=c):
                    line_arrival(sign, d, c).wait_recv()
                    if d < major - 1:
                        pl.when(onward(sign))(line(sign, d, c).start)
                    for o in range(1, minor):
                        if d == 1 and c in ends:
                            pl.when(jnp.logical_not(takes(sign)))(side(sign, d, o, c).start)
                        else:
                            side(sign, d, o, c).start()

            if d == 1 and c in ends:
                for sign in (1, -1):

                    @pl.when(gives(sign))
                    def _(sign=sign, c=c):
                        for o in range(1, minor):
                            side_arrival(1, 0, o, c).wait_recv()
                            to_pair(sign, o, c).start()

    for d in range(major):
        for sign in (1, -1) if d else (1,):

            @pl.when(held(sign, d))
            def _(sign=sign, d=d):
                for c in range(count):
                    for o in range(1, minor):
                        if c in ends and d == 0:
                            pl.when(gives(1))(to_pair(1, o, c).wait_send)
                            pl.when(gives(-1))(to_pair(-1, o, c).wait_send)
                            side(sign, d, o, c).wait_send()
                        elif c in ends and d == 1:

                            @pl.when(jnp.logical_not(takes(sign)))
                            def _(o=o, c=c):
                                side_arrival(sign, d, o, c).wait_recv()
                                side(sign, d, o, c).wait_send()

                            pl.when(takes(sign))(pair_arrival(sign, o, c).wait_recv)
                        else:
                            side_arrival(sign, d, o, c).wait_recv()
                            side(sign, d, o, c).wait_send()

        if d < major - 1:
            for sign in (1, -1):

                @pl.when(jnp.logical_and(held(sign, d), onward(sign)))
                def _(sign=sign, d=d):
                    for c in range(count):
                        line(sign, d, c).wait_send()

    for c in range(count):
        pltpu.make_async_copy(ins[c], at(c, me), local.at[c]).wait()


def gather(axis, n, minor, blocks, outs, dims, space, name):
    major = n // minor
    cut = 2
    arrays = len(blocks)
    count = arrays * cut
    sizes = tuple(b.shape[d] if o.ndim == 2 else 1 for b, o, d in zip(blocks, outs, dims))
    return pl.pallas_call(
        functools.partial(gather_kernel, axis, major, minor, cut, tuple(dims), sizes),
        out_shape=outs,
        in_specs=[pl.BlockSpec(memory_space=pltpu.VMEM)] * arrays,
        out_specs=[pl.BlockSpec(memory_space=space)] * arrays,
        scratch_shapes=[
            pltpu.SemaphoreType.DMA((count,)),
            pltpu.SemaphoreType.DMA((major, count)),
            pltpu.SemaphoreType.DMA((major, count)),
            pltpu.SemaphoreType.DMA((major, count)),
            pltpu.SemaphoreType.DMA((major, count)),
            pltpu.SemaphoreType.DMA((2 * major, minor, count)),
            pltpu.SemaphoreType.DMA((2 * major, minor, count)),
            pltpu.SemaphoreType.DMA((minor, count)),
            pltpu.SemaphoreType.DMA((minor, count)),
        ],
        compiler_params=pltpu.CompilerParams(collective_id=name, has_side_effects=True),
    )(*blocks)


def moment_kernel(n, parts, partial, first, second, first_new, second_new, portion,
                  arrived, squares, part_send, part_recv, square_send, square_recv, way_send, way_recv):
    me, col = lax.axis_index("fs"), lax.axis_index("tp")
    rows = first.shape[0]
    barrier = pltpu.get_barrier_semaphore()
    for k in range(1, n):
        pl.semaphore_signal(barrier, inc=1, device_id={"fs": (me + k) % n}, device_id_type=MESH)
    for k in range(1, parts):
        pl.semaphore_signal(barrier, inc=1, device_id={"tp": (col + k) % parts}, device_id_type=MESH)
    pl.semaphore_wait(barrier, n + parts - 2)

    def share(k):
        target = (me + k) % n
        return pltpu.make_async_remote_copy(
            src_ref=partial.at[pl.ds(pl.multiple_of(target * rows, 8), rows), :],
            dst_ref=arrived.at[k],
            send_sem=part_send.at[k],
            recv_sem=part_recv.at[k],
            device_id={"fs": target},
            device_id_type=MESH,
        )

    def square(axis, position, size, source, base, k):
        return pltpu.make_async_remote_copy(
            src_ref=squares.at[source],
            dst_ref=squares.at[base + k],
            send_sem=square_send.at[base + k],
            recv_sem=square_recv.at[base + k],
            device_id={axis: (position + k) % size},
            device_id_type=MESH,
        )

    for k in range(1, n):
        share(k).start()
    total = partial[pl.ds(pl.multiple_of(me * rows, 8), rows), :].astype(jnp.float32)
    for k in range(1, n):
        share(k).wait_recv()
        total = total + arrived[k].astype(jnp.float32)

    columns = jnp.sum(total * total, axis=0, keepdims=True)
    lanes = columns[:, :128]
    for j in range(1, columns.shape[1] // 128):
        lanes = lanes + columns[:, j * 128 : (j + 1) * 128]
    squares[0] = jnp.broadcast_to(lanes, squares.shape[1:])
    for k in range(1, parts):
        square("tp", col, parts, 0, 0, k).start()
    lanes = squares[0]
    for k in range(1, parts):
        square("tp", col, parts, 0, 0, k).wait_recv()
        lanes = lanes + squares[k]
    squares[parts] = lanes
    for k in range(1, n):
        square("fs", me, n, parts, parts, k).start()
    second_scaled = 0.95 * second[...]
    first_scaled = 0.8 * first[...]
    for k in range(1, n):
        square("fs", me, n, parts, parts, k).wait_recv()
        lanes = lanes + squares[parts + k]
    sum_squares = jnp.sum(lanes[:1], axis=1, keepdims=True)
    clip_factor = jnp.minimum(1.0, jnp.sqrt(3.0 * RANK * C_W / sum_squares))
    clipped = clip_factor * total
    first_value = first_scaled + 0.2 * clipped
    second_value = second_scaled + 0.05 * clipped * clipped
    mine = pl.ds(pl.multiple_of(me * rows, 8), rows)
    portion[mine, :] = (
        first_value * bias_first / (jnp.sqrt(second_value * bias_second) + 1e-08)
    ).astype(jnp.bfloat16)
    first_new[...] = first_value
    second_new[...] = second_value

    def way(k, owner):
        place = pl.ds(pl.multiple_of(owner * rows, 8), rows)
        return pltpu.make_async_remote_copy(
            src_ref=portion.at[place, :],
            dst_ref=portion.at[place, :],
            send_sem=way_send.at[k],
            recv_sem=way_recv.at[k],
            device_id={"fs": (me + k) % n},
            device_id_type=MESH,
        )

    for k in range(1, n):
        way(k, me).start()
    for k in range(1, n):
        share(k).wait_send()
        square("fs", me, n, parts, parts, k).wait_send()
    for k in range(1, parts):
        square("tp", col, parts, 0, 0, k).wait_send()
    for k in range(1, n):
        way(k, (me + n - k) % n).wait_recv()
        way(k, me).wait_send()


def moments(n, parts, partial, first, second):
    rows, width = first.shape
    return pl.pallas_call(
        functools.partial(moment_kernel, n, parts),
        out_shape=[
            jax.ShapeDtypeStruct(first.shape, jnp.float32),
            jax.ShapeDtypeStruct(first.shape, jnp.float32),
            jax.ShapeDtypeStruct(partial.shape, jnp.bfloat16),
        ],
        in_specs=[pl.BlockSpec(memory_space=pltpu.VMEM)] * 3,
        out_specs=[pl.BlockSpec(memory_space=pltpu.VMEM)] * 3,
        scratch_shapes=[
            pltpu.VMEM((n, rows, width), jnp.bfloat16),
            pltpu.VMEM((n + parts, 8, 128), jnp.float32),
            pltpu.SemaphoreType.DMA((n,)),
            pltpu.SemaphoreType.DMA((n,)),
            pltpu.SemaphoreType.DMA((n + parts,)),
            pltpu.SemaphoreType.DMA((n + parts,)),
            pltpu.SemaphoreType.DMA((n,)),
            pltpu.SemaphoreType.DMA((n,)),
        ],
        compiler_params=pltpu.CompilerParams(collective_id=3, has_side_effects=True),
    )(partial, first, second)


def body(
    n,
    parts,
    normed_input,
    query_cotangent,
    key_cotangent,
    head_outputs,
    output_cotangent,
    query_basis,
    key_basis,
    output_basis,
    query_master,
    key_master,
    output_master,
    query_first,
    query_second,
    key_first,
    key_second,
    output_first,
    output_second,
):
    width = query_cotangent.shape[1]
    tokens, depth = normed_input.shape
    bases = (query_basis, key_basis, output_basis)
    rank = query_basis.shape[1]
    piece = rank // parts
    minor = n // 4 if n % 4 == 0 else 1
    place = lax.axis_index("tp") * piece
    mine = jnp.concatenate(
        [lax.dynamic_slice_in_dim(b, place, piece, axis=1).T for b in bases], axis=0
    )
    (basis_rows,) = gather(
        "fs", n, minor, [mine], [jax.ShapeDtypeStruct((3 * piece, depth), jnp.bfloat16)], [1],
        pltpu.VMEM, 1,
    )
    contract = (((1,), (1,)), ((), ()))
    reduced = jnp.concatenate(
        [
            lax.dot_general(basis_rows[: 2 * piece], normed_input, contract,
                            preferred_element_type=jnp.float32),
            lax.dot_general(basis_rows[2 * piece :], output_cotangent, contract,
                            preferred_element_type=jnp.float32),
        ],
        axis=0,
    ).astype(jnp.bfloat16)
    (every,) = gather(
        "tp", parts, 2 if parts % 2 == 0 else 1, [reduced],
        [jax.ShapeDtypeStruct((parts, 3 * piece, tokens), jnp.bfloat16)], [0], pltpu.VMEM, 2,
    )
    right_sides = (query_cotangent, key_cotangent, head_outputs)
    partial_value = jnp.concatenate(
        [
            jnp.dot(
                every[:, member * piece : (member + 1) * piece].reshape(rank, tokens),
                right_sides[member],
                preferred_element_type=jnp.float32,
            ).astype(jnp.bfloat16)
            for member in range(3)
        ],
        axis=1,
    )
    first_moment = jnp.concatenate([query_first, key_first, output_first], axis=1)
    second_moment = jnp.concatenate([query_second, key_second, output_second], axis=1)
    first_new, second_new, portion = moments(n, parts, partial_value, first_moment, second_moment)
    query_update = 0.25 * jnp.dot(
        query_basis, portion[:, :width], preferred_element_type=jnp.float32
    )
    key_update = 0.25 * jnp.dot(
        key_basis, portion[:, width : 2 * width], preferred_element_type=jnp.float32
    )
    output_update = 0.25 * lax.dot_general(
        portion[:, 2 * width :], output_basis, (((0,), (1,)), ((), ())),
        preferred_element_type=jnp.float32,
    )
    query_master_new = query_master - learn_rate * (query_update + decay_rate * query_master)
    key_master_new = key_master - learn_rate * (key_update + decay_rate * key_master)
    output_master_new = output_master - learn_rate * (output_update + decay_rate * output_master)
    query_copy, key_copy, output_copy = gather(
        "fs", n, minor,
        [v.astype(jnp.bfloat16) for v in (query_master_new, key_master_new, output_master_new)],
        [
            jax.ShapeDtypeStruct((depth, width), jnp.bfloat16),
            jax.ShapeDtypeStruct((depth, width), jnp.bfloat16),
            jax.ShapeDtypeStruct((width, depth), jnp.bfloat16),
        ],
        [0, 0, 1], pl.ANY, 4,
    )
    return (
        query_master_new,
        key_master_new,
        output_master_new,
        query_copy,
        key_copy,
        output_copy,
        query_update.astype(jnp.bfloat16),
        key_update.astype(jnp.bfloat16),
        output_update.astype(jnp.bfloat16),
        first_new[:, :width],
        second_new[:, :width],
        first_new[:, width : 2 * width],
        second_new[:, width : 2 * width],
        first_new[:, 2 * width :],
        second_new[:, 2 * width :],
    )


def solution(mesh):
    placed = (
        P("fs", None),
        P("fs", "tp"),
        P("fs", "tp"),
        P("fs", "tp"),
        P("fs", None),
        P("fs", None),
        P("fs", None),
        P("fs", None),
        P("fs", "tp"),
        P("fs", "tp"),
        P("tp", "fs"),
        P("fs", "tp"),
        P("fs", "tp"),
        P("fs", "tp"),
        P("fs", "tp"),
        P("fs", "tp"),
        P("fs", "tp"),
    )
    return jax.shard_map(
        functools.partial(body, mesh.shape["fs"], mesh.shape["tp"]),
        mesh=mesh,
        in_specs=placed,
        out_specs=(
            P("fs", "tp"),
            P("fs", "tp"),
            P("tp", "fs"),
            P(None, "tp"),
            P(None, "tp"),
            P("tp", None),
            P("fs", "tp"),
            P("fs", "tp"),
            P("tp", "fs"),
            P("fs", "tp"),
            P("fs", "tp"),
            P("fs", "tp"),
            P("fs", "tp"),
            P("fs", "tp"),
            P("fs", "tp"),
        ),
        check_vma=False,
    )
```
